32 devices in a mesh: sp: 8 (over z, x), tp: 4 (over y, core).
Axes of the slice: x: 2, y: 2, z: 4, core: 2. Of those that a mesh axis runs over, the one named last changes fastest.
Arguments:
- queries: bfloat16 [1024, 2048], P('sp', 'tp'), may hold values from -15 to 15
- key_rows: bfloat16 [1024, 2048], P('sp', 'tp'), may hold values from -6 to 6
- value_rows: bfloat16 [1024, 2048], P('sp', 'tp'), may hold values from -6 to 6
- break_bias: bfloat16 [1024, 16], P('sp', 'tp'), may hold values from -14 to 1
- stream: bfloat16 [1024, 4096], P('sp', 'tp'), may hold values from -24 to 24
- out_proj: bfloat16 [2048, 4096], P(None, 'tp'), may hold values from -0.5 to 0.5
- norm_gain: float32 [4096], P('tp'), may hold values from 0.1 to 1.9
- expert_ids: int32 [1024, 2], P('sp'), may hold values from 0 to 15, all different within a row; in each aligned block of 128 rows (0 to 127, 128 to 255, ...) at most 32 rows name the same one
- route_weights: float32 [1024, 2], P('sp'), may hold values from 0.1 to 2.5
- gate_proj: bfloat16 [16, 4096, 384], P('sp', 'tp'), may hold values from -0.09375 to 0.09375
- up_proj: bfloat16 [16, 4096, 384], P('sp', 'tp'), may hold values from -0.09375 to 0.09375
- down_proj: bfloat16 [16, 384, 4096], P('sp', None, 'tp'), may hold values from -0.3125 to 0.3125
- shared_gate: bfloat16 [4096, 384], P('tp'), may hold values from -0.09375 to 0.09375
- shared_up: bfloat16 [4096, 384], P('tp'), may hold values from -0.09375 to 0.09375
- shared_down: bfloat16 [384, 4096], P(None, 'tp'), may hold values from -0.3125 to 0.3125
Outputs:
- result: bfloat16 [1024, 4096], P('sp', 'tp')
The draws below stay inside these ranges and needn't reach their ends.
Inputs may be any that keep to these rules, and one draw needn't show every extreme that they name: `expert_ids`: each row names 2 different experts; within the rows of one index of sp no expert is named by more than 32 rows, a bound that some block reaches of them.
All inputs are finite; a program needn't handle non-finite values.
Results may differ from the reference program's by a relative error of at most 0.022.
Values may be sent and summed in bfloat16 or wider, within the bound.
No kernel may reach another device: no remote copies, remote signals or barrier semaphores. Data moves between devices by JAX's collectives and lax.ppermute only.
A program may use at most 64 MiB of HBM per device.

```python
import math
import jax
import jax.numpy as jnp
import numpy as np
from jax import lax

D = 4096
ATTENTION_HEADS = 16
HD = 128
FFE = 384
FFS = 384
TOPK = 2
TOK_DEV = 128
SEQUENCE_TOKENS = 1024
EXPERTS = 16
CAP = 32
N_SP = 8
N_TP = 4


score_shift = 3.125


def draw_break_bias(key, part):
    every_key_rows = jax.random.split(jax.random.fold_in(key, 11), 5)
    fast_share = 0.5
    head_draw = jax.random.uniform(every_key_rows[0], (ATTENTION_HEADS,))
    fast_heads = head_draw < fast_share
    head_level = jnp.where(fast_heads, jnp.log(1.0 / 40.0), jnp.log(1.0 / SEQUENCE_TOKENS)) - score_shift
    block_shift = jax.random.uniform(every_key_rows[1], (SEQUENCE_TOKENS // TOK_DEV, ATTENTION_HEADS), minval=-0.7, maxval=0.7)
    jitter = 0.5 * jax.random.normal(every_key_rows[2], (SEQUENCE_TOKENS, ATTENTION_HEADS))
    logarithm_break_ratio = head_level[None, :] + jnp.repeat(block_shift, TOK_DEV, axis=0) + jitter
    stick_break_mask = jax.random.uniform(every_key_rows[3], (SEQUENCE_TOKENS, ATTENTION_HEADS)) < 4.0 / SEQUENCE_TOKENS
    break_probability = jax.random.uniform(every_key_rows[4], (SEQUENCE_TOKENS, ATTENTION_HEADS), minval=0.2, maxval=0.5)
    stick_break_level = jnp.log(break_probability / (1.0 - break_probability))
    return jnp.clip(jnp.where(stick_break_mask, stick_break_level, logarithm_break_ratio), -14.0, 1.0).astype(jnp.bfloat16)


def draw_stream(key, part):
    every_key_rows = jax.random.split(jax.random.fold_in(key, 23), 3)
    column_level = jnp.linspace(jnp.log(0.3), jnp.log(3.0), D) + 0.4 * jax.random.normal(every_key_rows[0], (D,))
    row_level = jax.random.uniform(every_key_rows[1], (SEQUENCE_TOKENS, 1), minval=jnp.log(0.15), maxval=jnp.log(1.5))
    base_values = jax.random.normal(every_key_rows[2], (SEQUENCE_TOKENS, D))
    scaled = base_values * jnp.exp(column_level)[None, :] * jnp.exp(row_level)
    return jnp.clip(scaled, -24.0, 24.0).astype(jnp.bfloat16)


def levels(rng, dims, shards, low, high):
    loudness, own = 1.0, jax.random.fold_in(rng, 6)
    for axis_at, blocks in shards:
        steps = jnp.exp(jax.random.uniform(jax.random.fold_in(own, axis_at), (blocks,), jnp.float32, low / len(shards), high / len(shards)))
        loudness = loudness * jnp.repeat(steps, dims[axis_at] // blocks).reshape([-1 if axis == axis_at else 1 for axis in range(len(dims))])
    return loudness


def deal_out(key, own, number, rows, amount, top, reach, lean):
    order = jax.random.permutation(key, amount)
    heavy_load, usual = shares(amount, rows * top, reach, lean, True), shares(amount, rows * top, reach, lean, False)
    places = jnp.arange(amount)

    def named(tallies, turn):
        used = int((tallies > 0).sum())
        fixed = max(1, used // 4)
        shifted = fixed + (places - fixed + turn * (used - fixed)) % max(1, amount - fixed)
        return jnp.zeros((amount,), jnp.int32).at[order[jnp.where(places < fixed, places, shifted)]].set(jnp.asarray(tallies, jnp.int32))

    tallies = jnp.where(number % 4 == 0, named(heavy_load, number // 4), named(usual, number - number // 4 - 1))
    mixed = jax.random.permutation(jax.random.fold_in(own, 3), amount)
    donor, receiver = mixed[0:amount // 2 * 2:2], mixed[1:amount // 2 * 2:2]
    room = jnp.minimum(tallies[donor] - 1, reach - tallies[receiver]) // 2
    room = jnp.where((donor == order[0]) | (receiver == order[0]) | (tallies[receiver] == 0), 0, jnp.maximum(room, 0))
    shifted = jax.random.randint(jax.random.fold_in(own, 4), (amount // 2,), 0, 1 << 20) % (room + 1)
    tallies = tallies.at[donor].add(-shifted).at[receiver].add(shifted)
    members = jnp.searchsorted(jnp.cumsum(tallies), jnp.arange(rows * top), side="right").astype(jnp.int32)
    table = members.reshape(top, rows).T
    table = table[jax.random.permutation(jax.random.fold_in(own, 1), rows)]
    turn = jax.random.randint(jax.random.fold_in(own, 2), (rows, 1), 0, top)
    return jnp.take_along_axis(table, (jnp.arange(top)[None, :] + turn) % top, axis=1)


def shares(number_of, total, bound, slope, full):
    portions = [(1 << 20) // math.isqrt(grade ** slope) + 1 for grade in range(1, number_of + 1)]
    largest = bound if full else min(bound, max(-(-total // number_of), total * portions[0] // sum(portions)))
    least = 1 if total - largest >= number_of - 1 else 0
    given, spare = [largest] + [least] * (number_of - 1), total - largest - least * (number_of - 1)
    while spare > 0:
        candidates = [i for i in range(1, number_of) if given[i] < largest] or [i for i in range(1, number_of) if given[i] < bound]
        pool, remaining = sum([portions[i] for i in candidates]), spare
        for i in candidates:
            more = min(bound - given[i], max(1, remaining * portions[i] // pool), spare)
            given[i] = given[i] + more
            spare = spare - more
    return np.array(given)


def normal_values(key, extent, deviation, bound, shards=(), held_as=jnp.bfloat16):
    loudness = levels(key, extent, shards, -0.22, 0.18) if shards else 1.0
    drawn = jax.random.normal(key, extent, jnp.float32) * deviation * loudness
    return jnp.minimum(jnp.maximum(drawn, -bound), bound).astype(held_as)


def setup_inputs(seed: int = 0) -> dict:
    streams_of = jax.random.split(jax.random.key(seed), 16)
    queries = normal_values(streams_of[0], (SEQUENCE_TOKENS, ATTENTION_HEADS * HD), 2.5, 15.0, ((0, 8), (1, 4)))
    key_rows = normal_values(streams_of[1], (SEQUENCE_TOKENS, ATTENTION_HEADS * HD), 1.0, 6.0, ((0, 8), (1, 4)))
    value_rows = normal_values(streams_of[2], (SEQUENCE_TOKENS, ATTENTION_HEADS * HD), 1.0, 6.0, ((0, 8), (1, 4)))
    break_bias = draw_break_bias(jax.random.fold_in(streams_of[15], 71), 0)
    stream = draw_stream(jax.random.fold_in(streams_of[15], 71), 0)
    out_proj = normal_values(streams_of[5], (ATTENTION_HEADS * HD, D), (ATTENTION_HEADS * HD // 16) ** -0.5, 0.5, ((1, 4),))
    norm_gain = jnp.clip(1.0 + 0.18 * jax.random.normal(streams_of[6], (D,), jnp.float32), 0.1, 1.9)
    expert_ids_keys = jax.random.split(jax.random.fold_in(streams_of[7], 1), SEQUENCE_TOKENS // TOK_DEV)
    expert_ids_turns = jax.random.permutation(jax.random.fold_in(streams_of[7], 3), SEQUENCE_TOKENS // TOK_DEV)
    expert_ids = jax.vmap(lambda own, number: deal_out(jax.random.fold_in(streams_of[7], 2), own, number, TOK_DEV, EXPERTS, TOPK, CAP, 2))(expert_ids_keys, expert_ids_turns).reshape((SEQUENCE_TOKENS, TOPK))
    route_weights = jnp.clip(jnp.exp(math.log(2.5) - 3.218876 * jax.random.uniform(streams_of[8], (SEQUENCE_TOKENS, TOPK), jnp.float32) ** levels(streams_of[8], (SEQUENCE_TOKENS, TOPK), ((0, 8),), -0.2, 0.2)), 0.1, 2.5)
    gate_proj = normal_values(streams_of[9], (EXPERTS, D, FFE), D ** -0.5, 0.09375, ((0, 8), (1, 4)))
    up_proj = normal_values(streams_of[10], (EXPERTS, D, FFE), D ** -0.5, 0.09375, ((0, 8), (1, 4)))
    down_proj = normal_values(streams_of[11], (EXPERTS, FFE, D), FFE ** -0.5, 0.3125, ((0, 8), (2, 4)))
    shared_gate = normal_values(streams_of[12], (D, FFS), D ** -0.5, 0.09375, ((0, 4),))
    shared_up = normal_values(streams_of[13], (D, FFS), D ** -0.5, 0.09375, ((0, 4),))
    shared_down = normal_values(streams_of[14], (FFS, D), FFS ** -0.5, 0.3125, ((1, 4),))
    return {"queries": queries, "key_rows": key_rows, "value_rows": value_rows, "break_bias": break_bias, "stream": stream, "out_proj": out_proj, "norm_gain": norm_gain, "expert_ids": expert_ids, "route_weights": route_weights, "gate_proj": gate_proj, "up_proj": up_proj, "down_proj": down_proj, "shared_gate": shared_gate, "shared_up": shared_up, "shared_down": shared_down}


EPS = 1e-06
query_block = 128

def stick_attention(queries, key_rows, value_rows, break_bias):
    head_q = queries.astype(jnp.float32).reshape(SEQUENCE_TOKENS, ATTENTION_HEADS, HD)
    head_k = key_rows.astype(jnp.float32).reshape(SEQUENCE_TOKENS, ATTENTION_HEADS, HD)
    head_v = value_rows.astype(jnp.float32).reshape(SEQUENCE_TOKENS, ATTENTION_HEADS, HD)
    bias_heads = break_bias.astype(jnp.float32).T
    key_pos = jnp.arange(SEQUENCE_TOKENS, dtype=jnp.int32)

    def one_block(block_index):
        offset = block_index * query_block
        query_part = lax.dynamic_slice_in_dim(head_q, offset, query_block, 0)
        positions = offset + jnp.arange(query_block, dtype=jnp.int32)
        logits = jnp.einsum('thd,shd->hts', query_part, head_k) * HD ** (-0.5) + bias_heads[:, None, :]
        before = (key_pos[None, :] < positions[:, None])[None]
        log_fail = jnp.where(before, jax.nn.log_sigmoid(-logits), 0.0)
        tail_sum = lax.cumsum(log_fail, axis=2, reverse=True) - log_fail
        weights = jnp.where(before, jnp.exp(jax.nn.log_sigmoid(logits) + tail_sum), 0.0)
        return jnp.einsum('hts,shd->thd', weights, head_v)
    outputs = lax.map(one_block, jnp.arange(SEQUENCE_TOKENS // query_block, dtype=jnp.int32))
    return outputs.reshape(SEQUENCE_TOKENS, ATTENTION_HEADS * HD).astype(jnp.bfloat16)

def block_sum(row_block, weight):
    feature_cut = row_block.shape[1] // N_TP

    def add_block(running, block_index):
        part_rows = lax.dynamic_slice_in_dim(row_block, block_index * feature_cut, feature_cut, 1)
        part_weight = lax.dynamic_slice_in_dim(weight, block_index * feature_cut, feature_cut, 0)
        partial_value = jnp.dot(part_rows, part_weight, preferred_element_type=jnp.float32).astype(jnp.bfloat16)
        partial_value = lax.optimization_barrier(partial_value)
        return (running + partial_value.astype(jnp.float32), None)
    start_sum = jnp.zeros((row_block.shape[0], weight.shape[1]), jnp.float32)
    running, _ = lax.scan(add_block, start_sum, jnp.arange(N_TP, dtype=jnp.int32))
    return running

def reference(queries, key_rows, value_rows, break_bias, stream, out_proj, norm_gain, expert_ids, route_weights, gate_proj, up_proj, down_proj, shared_gate, shared_up, shared_down):
    attended = stick_attention(queries, key_rows, value_rows, break_bias)
    mixed = (stream.astype(jnp.float32) + jnp.dot(attended, out_proj, preferred_element_type=jnp.float32)).astype(jnp.bfloat16)
    mixed = lax.optimization_barrier(mixed)
    mixed_f = mixed.astype(jnp.float32)
    inv_rms = lax.rsqrt(lax.optimization_barrier(jnp.mean(mixed_f * mixed_f, axis=1, keepdims=True)) + EPS)
    normed = (mixed_f * inv_rms * norm_gain[None, :]).astype(jnp.bfloat16)
    shared_hidden = (jax.nn.silu(block_sum(normed, shared_gate)) * block_sum(normed, shared_up)).astype(jnp.bfloat16)
    shared_out = jnp.dot(shared_hidden, shared_down, preferred_element_type=jnp.float32)
    rows_max = N_SP * CAP
    padded = jnp.concatenate([normed, jnp.zeros((1, D), jnp.bfloat16)], 0)

    def one_expert(running, expert):
        matches = expert_ids == expert
        chosen = jnp.any(matches, axis=1)
        weight_row = lax.optimization_barrier(jnp.sum(jnp.where(matches, route_weights, 0.0), axis=1))
        weight_pad = jnp.concatenate([weight_row, jnp.zeros((1,), jnp.float32)], 0)
        picked = jnp.nonzero(chosen, size=rows_max, fill_value=SEQUENCE_TOKENS)[0].astype(jnp.int32)
        row_block = padded[picked]
        gate_pre = block_sum(row_block, gate_proj[expert])
        up_pre = block_sum(row_block, up_proj[expert])
        hidden = (jax.nn.silu(gate_pre) * up_pre).astype(jnp.bfloat16)
        expert_out = jnp.dot(hidden, down_proj[expert], preferred_element_type=jnp.float32).astype(jnp.bfloat16)
        scaled = weight_pad[picked][:, None] * expert_out.astype(jnp.float32)
        return (running.at[picked].add(scaled), None)
    routed, _ = lax.scan(one_expert, jnp.zeros((SEQUENCE_TOKENS + 1, D), jnp.float32), jnp.arange(EXPERTS, dtype=jnp.int32))
    return (mixed_f + shared_out + routed[:SEQUENCE_TOKENS]).astype(jnp.bfloat16)
```

```python
import functools

import jax
import jax.numpy as jnp
from jax import lax
from jax.experimental import pallas as pl
from jax.experimental.pallas import tpu as pltpu
from jax.sharding import PartitionSpec as P

EPS = 1e-06
LANES = 128
BIAS_ROWS = 16
BF = jnp.bfloat16
F32 = jnp.float32


def vmem():
    return pl.BlockSpec(memory_space=pltpu.VMEM)


def smem():
    return pl.BlockSpec(memory_space=pltpu.SMEM)


def call(kernel, out_shape, in_specs, name, scratch=()):
    many = isinstance(out_shape, (tuple, list))
    return pl.pallas_call(
        kernel,
        out_shape=out_shape,
        in_specs=in_specs,
        out_specs=tuple(vmem() for _ in out_shape) if many else vmem(),
        scratch_shapes=list(scratch),
        name=name,
    )


def iota(shape, dim):
    return lax.broadcasted_iota(jnp.int32, shape, dim)


def dot(a, b):
    return jnp.dot(a, b, preferred_element_type=F32)


def split_pair(x):
    high = x.astype(BF)
    return high, (x - high.astype(F32)).astype(BF)


def pack_kernel(q_ref, k_ref, v_ref, b_ref, out_ref, *, heads, group, rows, hd):
    tok = k_ref.shape[0]
    bias_t = jnp.transpose(b_ref[...].astype(F32))
    for h in range(heads):
        cols = slice(h * hd, (h + 1) * hd)
        bias = jnp.broadcast_to(bias_t[h : h + 1, :], (BIAS_ROWS, tok)).astype(BF)
        for p in range(group):
            s = h * group + p
            out_ref[s, 0:tok] = k_ref[:, cols]
            out_ref[s, tok : 2 * tok] = v_ref[:, cols]
            out_ref[s, 2 * tok : 2 * tok + BIAS_ROWS] = bias
            out_ref[s, 2 * tok + BIAS_ROWS :] = q_ref[p * rows : (p + 1) * rows, cols]


def pack_plain(q, k, v, b, heads, group, rows, padded_rows, hd):
    tok = k.shape[0]
    kh = k.reshape(tok, heads, hd).transpose(1, 0, 2)
    vh = v.reshape(tok, heads, hd).transpose(1, 0, 2)
    bh = jnp.broadcast_to(b.T[:, None, :], (heads, BIAS_ROWS, tok))
    both = jnp.concatenate([kh, vh, bh], axis=1)
    both = jnp.broadcast_to(both[:, None], (heads, group) + both.shape[1:])
    qh = q.reshape(group, rows, heads, hd).transpose(2, 0, 1, 3)
    qh = jnp.pad(qh, ((0, 0), (0, 0), (0, padded_rows - rows), (0, 0)))
    return jnp.concatenate([both, qh], axis=2).reshape(heads * group, -1, hd)


def attention_kernel(p_ref, x_ref, out_ref, acc_ref, carry_ref, *, rows, padded, hd, tok):
    blocks = x_ref.shape[0]
    q0 = 2 * tok + BIAS_ROWS
    queries = jnp.concatenate([x_ref[i, q0 : q0 + padded] for i in range(blocks)], axis=0)
    acc_ref[...] = jnp.zeros_like(acc_ref)
    carry_ref[...] = jnp.zeros_like(carry_ref)
    src = iota((2 * tok, 2 * tok), 0)
    src = jnp.where(src >= tok, src - tok, src)
    dst = iota((2 * tok, 2 * tok), 1)
    tri = jnp.where((dst >= tok) | (src > dst), 1.0, 0.0).astype(BF)
    first = p_ref[0] * rows
    scale = hd ** (-0.5)
    for j in reversed(range(blocks)):
        r0 = j * padded
        n = blocks * padded - r0
        keys = x_ref[j, 0:tok]
        values = x_ref[j, tok : 2 * tok]
        bias = x_ref[j, 2 * tok : 2 * tok + BIAS_ROWS].astype(F32)[0:1, :]
        raw = lax.dot_general(
            queries[r0:, :], keys, (((1,), (1,)), ((), ())), preferred_element_type=F32
        )
        logits = raw * scale + bias
        soft = jnp.log(1.0 + jnp.exp(-jnp.abs(logits)))
        fail = -(jnp.maximum(logits, 0.0) + soft)
        row = iota((n, tok), 0)
        before = (row >= padded) | (iota((n, tok), 1) < row + first)
        stay = logits + fail
        fail = jnp.where(before, fail, 0.0)
        high, low = split_pair(fail)
        sums = dot(jnp.concatenate([high, low], axis=1), tri)
        carry = carry_ref[r0:, :]
        weights = jnp.where(before, jnp.exp(stay + sums[:, :tok] + carry), 0.0)
        carry_ref[r0:, :] = carry + sums[:, tok:]
        acc_ref[r0:, :] += dot(weights.astype(BF), values)
    out_ref[...] = acc_ref[...].astype(BF).reshape(out_ref.shape)


def project_kernel(t_ref, ids_ref, *refs, masks, heads, group, rows, cap, arranged):
    count = len(masks)
    pieces = refs[:count]
    w_ref, stream_ref, mixed_ref, send_ref = refs[count:]
    t = t_ref[0]
    total = stream_ref[...].astype(F32)
    for mask, piece in zip(masks, pieces):
        if arranged:
            part = piece[...]
        else:
            part = jnp.concatenate(
                [
                    jnp.concatenate([piece[h * group + p] for p in range(group)], axis=0)
                    for h in range(heads)
                ],
                axis=1,
            )
        total = total + dot(part, w_ref[jnp.bitwise_xor(t, mask)])
    mixed = total.astype(BF)
    mixed_ref[...] = mixed
    tok = mixed.shape[0]
    experts = send_ref.shape[0] // cap
    named = [iota((experts, tok), 0) == ids_ref[k : k + 1, :] for k in range(ids_ref.shape[0])]
    hit = functools.reduce(jnp.logical_or, named)
    order = jnp.where(iota((tok, tok), 0) < iota((tok, tok), 1), 1.0, 0.0).astype(BF)
    rank = dot(jnp.where(hit, 1.0, 0.0).astype(BF), order)
    rank = jnp.where(hit, rank, -1.0)
    slot = iota((cap, tok), 0).astype(F32)
    pick = jnp.concatenate(
        [jnp.where(slot == rank[e : e + 1, :], 1.0, 0.0) for e in range(experts)], axis=0
    )
    send_ref[...] = dot(pick.astype(BF), mixed).astype(BF)


def partials(x, gain, gate, up):
    scaled = (x * gain).astype(BF)
    square = jnp.sum(x * x, axis=1, keepdims=True)
    high, low = split_pair(square)
    lane = iota((x.shape[0], LANES), 1)
    tail = jnp.where(lane == 0, high.astype(F32), jnp.where(lane == 1, low.astype(F32), 0.0))
    return jnp.concatenate(
        [dot(scaled, gate).astype(BF), dot(scaled, up).astype(BF), tail.astype(BF)], axis=1
    )


def shared_kernel(mixed_ref, gain_ref, gate_ref, up_ref, out_ref):
    out_ref[...] = partials(
        mixed_ref[...].astype(F32), gain_ref[...], gate_ref[...], up_ref[...]
    )


def routed_kernel(e_ref, x_ref, gain_ref, gate_ref, up_ref, out_ref):
    x = x_ref[...].astype(F32)
    x = x.reshape(-1, x.shape[-1])
    out_ref[...] = partials(x, gain_ref[...], gate_ref[0], up_ref[0])


def add_partials(a_ref, b_ref, width):
    a = a_ref[...].astype(F32)
    b = b_ref[...].astype(F32)
    body = a[:, :width] + b[:, :width]
    square = a[:, width : width + 1] + b[:, width : width + 1]
    square = square + (a[:, width + 1 : width + 2] + b[:, width + 1 : width + 2])
    return body, square


def add_kernel(a_ref, b_ref, out_ref, *, width):
    body, square = add_partials(a_ref, b_ref, width)
    high, low = split_pair(square)
    lane = iota((body.shape[0], LANES), 1)
    tail = jnp.where(lane == 0, high.astype(F32), jnp.where(lane == 1, low.astype(F32), 0.0))
    out_ref[...] = jnp.concatenate([body.astype(BF), tail.astype(BF)], axis=1)


def hidden_kernel(a_ref, b_ref, out_ref, *, width, features):
    body, square = add_partials(a_ref, b_ref, width)
    inv = lax.rsqrt(square / features + EPS)
    gate = body[:, : width // 2] * inv
    up = body[:, width // 2 :] * inv
    out_ref[...] = (gate * jax.nn.sigmoid(gate) * up).astype(BF)


def down_kernel(c_ref, own_ref, other_ref, w_ref, out_ref):
    c = c_ref[0]
    blocks, _, cap, feats = out_ref.shape
    out_ref[:, pl.ds(c, 1)] = dot(own_ref[...], w_ref[c]).reshape(blocks, 1, cap, feats).astype(BF)
    d = 1 - c
    out_ref[:, pl.ds(d, 1)] = (
        dot(other_ref[...], w_ref[d]).reshape(blocks, 1, cap, feats).astype(BF)
    )


def combine_kernel(ids_ref, rw_ref, back_ref, mixed_ref, hid_ref, down_ref, out_ref, *, cap):
    tok, choices = ids_ref.shape
    slots = back_ref.shape[0]
    experts = slots // cap
    ids = ids_ref[...]
    named = [iota((tok, experts), 1) == ids[:, k : k + 1] for k in range(choices)]
    hit = functools.reduce(jnp.logical_or, named)
    order = jnp.where(iota((tok, tok), 1) < iota((tok, tok), 0), 1.0, 0.0).astype(BF)
    rank = dot(order, jnp.where(hit, 1.0, 0.0).astype(BF))
    place = rank + (iota((tok, experts), 1) * cap).astype(F32)
    lane = iota((tok, slots), 1).astype(F32)
    pick = jnp.zeros((tok, slots), F32)
    for k in range(choices):
        at = jnp.sum(jnp.where(named[k], place, 0.0), axis=1, keepdims=True)
        pick = pick + jnp.where(lane == at, rw_ref[:, k : k + 1], 0.0)
    high, low = split_pair(pick)
    back = back_ref[...]
    total = mixed_ref[...].astype(F32) + dot(hid_ref[...], down_ref[...])
    total = total + (dot(high, back) + dot(low, back))
    out_ref[...] = total.astype(BF)


def swap(x, axis, bit):
    count = lax.axis_size(axis)
    return lax.ppermute(x, axis, [(i, i ^ bit) for i in range(count)])


def body(
    queries,
    key_rows,
    value_rows,
    break_bias,
    stream,
    out_proj,
    norm_gain,
    expert_ids,
    route_weights,
    gate_proj,
    up_proj,
    down_proj,
    shared_gate,
    shared_up,
    shared_down,
):
    tok = queries.shape[0]
    heads = break_bias.shape[1]
    hd = queries.shape[1] // heads
    blocks = lax.axis_size("sp")
    tp = lax.axis_size("tp")
    feats = stream.shape[1]
    features = feats * tp
    s_index = lax.axis_index("sp")
    t_index = lax.axis_index("tp")
    group = blocks // heads
    rows = tok // group
    padded = max(rows, 16)
    aligned = rows % 16 == 0

    if aligned:
        packed = call(
            functools.partial(pack_kernel, heads=heads, group=group, rows=rows, hd=hd),
            jax.ShapeDtypeStruct((blocks, 2 * tok + BIAS_ROWS + padded, hd), BF),
            [vmem()] * 4,
            "pack",
        )(queries, key_rows, value_rows, break_bias)
    else:
        packed = pack_plain(
            queries, key_rows, value_rows, break_bias, heads, group, rows, padded, hd
        )
    moved = lax.all_to_all(packed, "sp", 0, 0, tiled=True)
    part_index = (s_index % group).astype(jnp.int32).reshape(1)
    attended = call(
        functools.partial(attention_kernel, rows=rows, padded=padded, hd=hd, tok=tok),
        jax.ShapeDtypeStruct((blocks, padded, hd), BF),
        [smem(), vmem()],
        "attention",
        [pltpu.VMEM((blocks * padded, hd), F32), pltpu.VMEM((blocks * padded, tok), F32)],
    )(part_index, moved)
    piece = lax.all_to_all(attended, "sp", 0, 0, tiled=True)
    if not aligned:
        piece = piece.reshape(heads, group, padded, hd)[:, :, :rows]
        piece = piece.transpose(1, 2, 0, 3).reshape(tok, heads * hd)
    bits = [1 << i for i in range(tp.bit_length() - 1)]
    pieces, masks = [piece], [0]
    for bit in reversed(bits):
        pieces = pieces + [swap(x, "tp", bit) for x in pieces]
        masks = masks + [m ^ bit for m in masks]

    experts_local = gate_proj.shape[0]
    experts = experts_local * blocks
    choices = expert_ids.shape[1]
    cap = 2 * choices * tok // experts
    t_array = t_index.astype(jnp.int32).reshape(1)
    mixed, send = call(
        functools.partial(
            project_kernel,
            masks=tuple(masks),
            heads=heads,
            group=group,
            rows=rows,
            cap=cap,
            arranged=not aligned,
        ),
        (
            jax.ShapeDtypeStruct((tok, feats), BF),
            jax.ShapeDtypeStruct((experts * cap, feats), BF),
        ),
        [smem()] + [vmem()] * (len(pieces) + 3),
        "project",
    )(t_array, expert_ids.T, *pieces, out_proj.reshape(tp, -1, feats), stream)
    arrived = lax.all_to_all(
        send.reshape(blocks, experts_local, cap, feats), "sp", 0, 0, tiled=True
    )

    gain = norm_gain.reshape(1, feats)
    hid_s = shared_gate.shape[1]
    shared_sum = call(
        shared_kernel,
        jax.ShapeDtypeStruct((tok, 2 * hid_s + LANES), BF),
        [vmem()] * 4,
        "shared",
    )(mixed, gain, shared_gate, shared_up)

    def add(a, b, width):
        return call(
            functools.partial(add_kernel, width=width),
            jax.ShapeDtypeStruct(a.shape, BF),
            [vmem()] * 2,
            "add",
        )(a, b)

    def hidden(a, b, width):
        return call(
            functools.partial(hidden_kernel, width=width, features=features),
            jax.ShapeDtypeStruct((a.shape[0], width // 2), BF),
            [vmem()] * 2,
            "hidden",
        )(a, b)

    for bit in bits[:-1]:
        shared_sum = add(shared_sum, swap(shared_sum, "tp", bit), 2 * hid_s)
    shared_hidden = hidden(shared_sum, swap(shared_sum, "tp", bits[-1]), 2 * hid_s)

    hid_r = gate_proj.shape[2]
    expert_rows = blocks * cap

    def routed(e):
        spec = pltpu.PrefetchScalarGridSpec(
            num_scalar_prefetch=1,
            grid=(1,),
            in_specs=[
                pl.BlockSpec((blocks, 1, cap, feats), lambda i, e: (0, e[0], 0, 0)),
                pl.BlockSpec((1, feats), lambda i, e: (0, 0)),
                pl.BlockSpec((1, feats, hid_r), lambda i, e: (e[0], 0, 0)),
                pl.BlockSpec((1, feats, hid_r), lambda i, e: (e[0], 0, 0)),
            ],
            out_specs=pl.BlockSpec((expert_rows, 2 * hid_r + LANES), lambda i, e: (0, 0)),
        )
        return pl.pallas_call(
            routed_kernel,
            out_shape=jax.ShapeDtypeStruct((expert_rows, 2 * hid_r + LANES), BF),
            grid_spec=spec,
            name="routed",
        )(e, arrived, gain, gate_proj, up_proj)

    core = t_array % 2
    away = routed(1 - core)
    came = swap(away, "tp", 1)
    total = add(routed(core), came, 2 * hid_r)
    for bit in bits[1:-1]:
        total = add(total, swap(total, "tp", bit), 2 * hid_r)
    hid_own = hidden(total, swap(total, "tp", bits[-1]), 2 * hid_r)
    hid_other = swap(hid_own, "tp", 1)
    outs = call(
        down_kernel,
        jax.ShapeDtypeStruct((blocks, experts_local, cap, feats), BF),
        [smem()] + [vmem()] * 3,
        "down",
    )(core, hid_own, hid_other, down_proj)
    back = lax.all_to_all(outs, "sp", 0, 0, tiled=True).reshape(experts * cap, feats)
    return call(
        functools.partial(combine_kernel, cap=cap),
        jax.ShapeDtypeStruct((tok, feats), BF),
        [vmem()] * 6,
        "combine",
    )(expert_ids, route_weights, back, mixed, shared_hidden, shared_down)


def solution(mesh):
    in_specs = (
        P("sp", "tp"),
        P("sp", "tp"),
        P("sp", "tp"),
        P("sp", "tp"),
        P("sp", "tp"),
        P(None, "tp"),
        P("tp"),
        P("sp", None),
        P("sp", None),
        P("sp", "tp", None),
        P("sp", "tp", None),
        P("sp", None, "tp"),
        P("tp", None),
        P("tp", None),
        P(None, "tp"),
    )
    out_specs = P("sp", "tp")
    return jax.shard_map(body, mesh=mesh, in_specs=in_specs, out_specs=out_specs, check_vma=False)
```

```python
import functools

import jax
import jax.numpy as jnp
from jax import lax
from jax.experimental import pallas as pl
from jax.experimental.pallas import tpu as pltpu
from jax.sharding import PartitionSpec as P


EPS = 1e-06
LANES = 128
BIAS_ROWS = 16
VMEM_LIMIT = 16 * 1024 * 1024
BF = jnp.bfloat16
F32 = jnp.float32


def vmem():
    return pl.BlockSpec(memory_space=pltpu.VMEM)


def hbm():
    return pl.BlockSpec(memory_space=pltpu.HBM)


def in_hbm(x):
    return pltpu.with_memory_space_constraint(x, pltpu.HBM)


def smem():
    return pl.BlockSpec(memory_space=pltpu.SMEM)


def call(kernel, out_shape, in_specs, scratch=()):
    many = isinstance(out_shape, (tuple, list))
    return pl.pallas_call(
        kernel,
        out_shape=out_shape,
        in_specs=in_specs,
        out_specs=tuple(vmem() for _ in out_shape) if many else vmem(),
        scratch_shapes=list(scratch),
        compiler_params=pltpu.CompilerParams(vmem_limit_bytes=VMEM_LIMIT),
    )


def iota(shape, dim):
    return lax.broadcasted_iota(jnp.int32, shape, dim)


def dot(a, b):
    return jnp.dot(a, b, preferred_element_type=F32)


def split_pair(x):
    high = x.astype(BF)
    return high, (x - high.astype(F32)).astype(BF)


def pack_kernel(at_ref, q_ref, k_ref, v_ref, b_ref, *refs, hd):
    outs, sems = refs[:-1], refs[-1]
    tok = k_ref.shape[0]
    copies = []
    for mh, out in enumerate(outs):
        head = jnp.bitwise_xor(at_ref[0], mh)
        cols = pl.ds(pl.multiple_of(head * hd, hd), hd)
        for i, (src, start) in enumerate(
            ((k_ref, 0), (v_ref, tok), (q_ref, 2 * tok + BIAS_ROWS))
        ):
            copy = pltpu.make_async_copy(
                src.at[:, cols], out.at[pl.ds(start, tok)], sems.at[3 * mh + i]
            )
            copy.start()
            copies.append(copy)
    bias = b_ref[...].astype(F32)
    for mh, out in enumerate(outs):
        head = jnp.bitwise_xor(at_ref[0], mh)
        row = jnp.where(iota(bias.shape, 0) == head, bias, 0.0)
        row = jnp.sum(row, axis=0, keepdims=True)
        out[2 * tok : 2 * tok + BIAS_ROWS] = jnp.broadcast_to(row, (BIAS_ROWS, tok)).astype(BF)
    for copy in copies:
        copy.wait()


def attention_kernel(at_ref, w_hbm, *refs, heads, group):
    blocks = heads * group
    ins, outs = refs[:blocks], refs[blocks : blocks + heads]
    w_ref, kv_ref, q_ref, acc_ref, carry_ref, sem = refs[blocks + heads :]
    fetch = pltpu.make_async_copy(w_hbm, w_ref, sem)
    fetch.start()
    rows, hd = ins[0].shape
    kv_rows = kv_ref.shape[1]
    tok = rows - kv_rows
    h, p = at_ref[0], at_ref[1]
    for mh in range(heads):
        g = jnp.bitwise_xor(h, mh)
        q_ref[pl.ds(pl.multiple_of(g * tok, tok), tok)] = ins[mh * group][kv_rows:]
        for mp in range(group):
            kv_ref[g * group + jnp.bitwise_xor(p, mp)] = ins[mh * group + mp][:kv_rows]
    acc_ref[...] = jnp.zeros_like(acc_ref)
    carry_ref[...] = jnp.zeros_like(carry_ref)
    src = iota((2 * tok, 2 * tok), 0)
    src = jnp.where(src >= tok, src - tok, src)
    dst = iota((2 * tok, 2 * tok), 1)
    tri = jnp.where((dst >= tok) | (src > dst), 1.0, 0.0).astype(BF)
    scale = hd ** (-0.5)
    for j in reversed(range(blocks)):
        r0 = (j // group) * tok
        n = heads * tok - r0
        keys = kv_ref[j, 0:tok]
        values = kv_ref[j, tok : 2 * tok]
        bias = kv_ref[j, 2 * tok : 2 * tok + BIAS_ROWS].astype(F32)[0:1, :]
        raw = lax.dot_general(
            q_ref[r0:], keys, (((1,), (1,)), ((), ())), preferred_element_type=F32
        )
        logits = raw * scale + bias
        soft = jnp.log(1.0 + jnp.exp(-jnp.abs(logits)))
        fail = -(jnp.maximum(logits, 0.0) + soft)
        row = iota((n, tok), 0)
        before = (row >= tok) | (iota((n, tok), 1) < row + (p - j % group) * tok)
        stay = logits + fail
        fail = jnp.where(before, fail, 0.0)
        high, low = split_pair(fail)
        sums = dot(jnp.concatenate([high, low], axis=1), tri)
        carry = carry_ref[r0:]
        weights = jnp.where(before, jnp.exp(stay + sums[:, :tok] + carry), 0.0)
        carry_ref[r0:] = carry + sums[:, tok:]
        acc_ref[r0:] += dot(weights.astype(BF), values)
    for mh in range(heads):
        g = jnp.bitwise_xor(h, mh)
        outs[mh][...] = acc_ref[pl.ds(pl.multiple_of(g * tok, tok), tok)].astype(BF)
    fetch.wait()


def stack_kernel(*refs):
    for i, ref in enumerate(refs[:-1]):
        refs[-1][i] = ref[...]


def slots_of(ids_ref, s, c, local, blocks):
    tok = ids_ref.shape[1]
    expert = jnp.bitwise_xor(iota((blocks, tok), 0), s) * local + c
    named = [expert == ids_ref[k : k + 1, :] for k in range(ids_ref.shape[0])]
    hit = functools.reduce(jnp.logical_or, named)
    order = jnp.where(iota((tok, tok), 0) < iota((tok, tok), 1), 1.0, 0.0).astype(BF)
    rank = dot(jnp.where(hit, 1.0, 0.0).astype(BF), order)
    return named, jnp.where(hit, rank, -1.0)


def spread(rank, values, cap):
    slot = iota((cap, rank.shape[1]), 0).astype(F32)
    return jnp.concatenate(
        [
            jnp.where(slot == rank[e : e + 1, :], values[e : e + 1, :], 0.0)
            for e in range(rank.shape[0])
        ],
        axis=0,
    )


def project_kernel(at_ref, *refs, masks, heads):
    count = len(masks)
    pieces = refs[:count]
    w_ref, stream_ref, mixed_ref, rows_ref = refs[count:]
    h, t = at_ref[0], at_ref[2]
    for mask, piece in zip(masks, pieces):
        hd = piece.shape[2]
        for mh in range(heads):
            head = jnp.bitwise_xor(t, mask) * heads + jnp.bitwise_xor(h, mh)
            rows_ref[:, pl.ds(pl.multiple_of(head * hd, hd), hd)] = piece[mh]
    total = stream_ref[...].astype(F32) + dot(rows_ref[...], w_ref[...])
    mixed_ref[...] = total.astype(BF)


def dispatch_kernel(at_ref, ids_ref, own_ref, other_ref, *sends, local):
    cap = sends[0].shape[1]
    _, rank = slots_of(ids_ref, at_ref[3], at_ref[4], local, len(sends))
    pick = spread(rank, jnp.ones_like(rank), cap).astype(BF)
    for side, ref in enumerate((own_ref, other_ref)):
        rows = dot(pick, ref[...]).astype(BF)
        for m, send in enumerate(sends):
            send[side] = rows[m * cap : (m + 1) * cap]


def square_lanes(square):
    high, low = split_pair(square)
    lane = iota((square.shape[0], LANES), 1)
    tail = jnp.where(lane == 0, high.astype(F32), jnp.where(lane == 1, low.astype(F32), 0.0))
    return tail.astype(BF)


def partials(sides):
    gate_sum, up_sum, square = 0.0, 0.0, 0.0
    for x, gain, gate, up in sides:
        scaled = (x * gain).astype(BF)
        square = square + jnp.sum(x * x, axis=1, keepdims=True)
        gate_sum = gate_sum + dot(scaled, gate).astype(BF).astype(F32)
        up_sum = up_sum + dot(scaled, up).astype(BF).astype(F32)
    return jnp.concatenate(
        [gate_sum.astype(BF), up_sum.astype(BF), square_lanes(square)], axis=1
    )


def shared_kernel(mixed_ref, gain_ref, gate_ref, up_ref, out_ref):
    out_ref[...] = partials(
        [(mixed_ref[...].astype(F32), gain_ref[...], gate_ref[...], up_ref[...])]
    )


def routed_kernel(at_ref, *refs):
    e = at_ref[4]
    weights, out_ref = refs[-7:-1], refs[-1]
    sides = []
    for side in range(2):
        x = jnp.concatenate([ref[side].astype(F32) for ref in refs[:-7]], axis=0)
        gain_ref, gate_ref, up_ref = weights[3 * side : 3 * side + 3]
        sides.append((x, gain_ref[...], gate_ref[e], up_ref[e]))
    out_ref[...] = partials(sides)


def add_partials(a_ref, b_ref, width):
    a = a_ref[...].astype(F32)
    b = b_ref[...].astype(F32)
    body = a[:, :width] + b[:, :width]
    square = a[:, width : width + 1] + b[:, width : width + 1]
    square = square + (a[:, width + 1 : width + 2] + b[:, width + 1 : width + 2])
    return body, square


def add_kernel(a_ref, b_ref, out_ref, *, width):
    body, square = add_partials(a_ref, b_ref, width)
    out_ref[...] = jnp.concatenate([body.astype(BF), square_lanes(square)], axis=1)


def hidden_of(a_ref, b_ref, width, features):
    body, square = add_partials(a_ref, b_ref, width)
    inv = lax.rsqrt(square / features + EPS)
    gate = body[:, : width // 2] * inv
    up = body[:, width // 2 :] * inv
    return (gate * jax.nn.sigmoid(gate) * up).astype(BF)


def hidden_kernel(a_ref, b_ref, out_ref, *, width, features):
    out_ref[...] = hidden_of(a_ref, b_ref, width, features)


def down_kernel(at_ref, a_ref, b_ref, own_ref, other_ref, *outs, width, features):
    hidden = hidden_of(a_ref, b_ref, width, features)
    cap = outs[0].shape[1]
    for side, w_ref in enumerate((own_ref, other_ref)):
        rows = dot(hidden, w_ref[at_ref[4]]).astype(BF)
        for i, out in enumerate(outs):
            out[side] = rows[i * cap : (i + 1) * cap]


def base_kernel(at_ref, ids_ref, rw_ref, mixed_ref, hid_ref, down_ref, base_ref, *picks, local, cap):
    blocks = sum(pick.shape[1] for pick in picks) // (2 * cap)
    named, rank = slots_of(ids_ref, at_ref[3], at_ref[4], local, blocks)
    weight = functools.reduce(
        jnp.add,
        [jnp.where(hit, rw_ref[k : k + 1, :], 0.0) for k, hit in enumerate(named)],
    )
    high, low = split_pair(jnp.transpose(spread(rank, weight, cap)))
    start = 0
    for pick in picks:
        width = pick.shape[1] // 2
        pick[:, :width] = high[:, start : start + width]
        pick[:, width:] = low[:, start : start + width]
        start += width
    base_ref[0] = mixed_ref[...].astype(F32) + dot(hid_ref[...], down_ref[...])
    base_ref[1] = jnp.zeros_like(base_ref[1])


def combine_kernel(base_ref, pick_ref, *refs, outs):
    backs, out_refs = refs[:-outs], refs[-outs:]
    for side in range(2):
        rows = jnp.concatenate([ref[side] for ref in backs], axis=0)
        rows = jnp.concatenate([rows, rows], axis=0)
        total = base_ref[side] + dot(pick_ref[...], rows)
        if outs == 1:
            out_refs[0][side] = total
        else:
            out_refs[side][...] = total


def final_kernel(a_ref, b_ref, out_ref):
    out_ref[...] = (a_ref[...] + b_ref[...]).astype(BF)


def swap(x, axis, bit):
    if bit == 0:
        return x
    count = lax.axis_size(axis)
    return lax.ppermute(x, axis, [(i, i ^ bit) for i in range(count)])


def layer(
    queries,
    key_rows,
    value_rows,
    break_bias,
    stream,
    out_proj,
    norm_gain,
    expert_ids,
    route_weights,
    gate_proj,
    up_proj,
    down_proj,
    shared_gate,
    shared_up,
    shared_down,
):
    tok = queries.shape[0]
    heads = break_bias.shape[1]
    hd = queries.shape[1] // heads
    blocks = lax.axis_size("sp")
    tp = lax.axis_size("tp")
    feats = stream.shape[1]
    features = feats * tp
    s_index = lax.axis_index("sp").astype(jnp.int32)
    t_index = lax.axis_index("tp").astype(jnp.int32)
    group = blocks // heads
    h_index, p_index = s_index // group, s_index % group

    def array(*shape):
        return jax.ShapeDtypeStruct(shape, BF)

    at = jnp.stack([h_index, p_index, t_index, s_index, t_index % 2])
    rows = 3 * tok + BIAS_ROWS
    gain = norm_gain.reshape(1, feats)
    others = [swap(x, "tp", 1) for x in (gain, gate_proj, up_proj, down_proj)]
    packed = call(
        functools.partial(pack_kernel, hd=hd),
        (array(rows, hd),) * heads,
        [smem()] + [hbm()] * 3 + [vmem()],
        [pltpu.SemaphoreType.DMA((3 * heads,))],
    )(at, in_hbm(queries), in_hbm(key_rows), in_hbm(value_rows), break_bias.T)
    qkv = [swap(packed[mh], "sp", mh * group) for mh in range(heads)]
    qkv = [swap(qkv[mh], "sp", mp) for mh in range(heads) for mp in range(group)]
    *attended, out_w = call(
        functools.partial(attention_kernel, heads=heads, group=group),
        (array(tok, hd),) * heads + (array(*out_proj.shape),),
        [smem(), hbm()] + [vmem()] * blocks,
        [
            pltpu.VMEM((blocks, rows - tok, hd), BF),
            pltpu.VMEM((heads * tok, hd), BF),
            pltpu.VMEM((heads * tok, hd), F32),
            pltpu.VMEM((heads * tok, tok), F32),
            pltpu.SemaphoreType.DMA,
        ],
    )(at, in_hbm(out_proj), *qkv)
    piece = call(stack_kernel, array(heads, tok, hd), [vmem()] * heads)(
        *[swap(attended[mh], "sp", mh * group) for mh in range(heads)]
    )
    bits = [1 << i for i in range(tp.bit_length() - 1)]
    pieces, masks = [piece], [0]
    for bit in reversed(bits):
        pieces = pieces + [swap(x, "tp", bit) for x in pieces]
        masks = masks + [m ^ bit for m in masks]

    local = gate_proj.shape[0]
    experts = local * blocks
    choices = expert_ids.shape[1]
    cap = 2 * choices * tok // experts
    mixed = call(
        functools.partial(project_kernel, masks=tuple(masks), heads=heads),
        array(tok, feats),
        [smem()] + [vmem()] * (len(pieces) + 2),
        [pltpu.VMEM((tok, out_proj.shape[0]), BF)],
    )(at, *pieces, out_w, stream)
    mixed_other = swap(mixed, "tp", 1)
    sends = call(
        functools.partial(dispatch_kernel, local=local),
        (array(2, cap, feats),) * blocks,
        [smem()] + [vmem()] * 3,
    )(at, expert_ids.T, mixed, mixed_other)

    half = blocks // 2
    quarter = half + half // 2
    groups = [range(half), range(half, quarter), range(quarter, blocks)]
    arrived = {m: swap(sends[m], "sp", m) for m in range(blocks)}

    hid_s = shared_gate.shape[1]
    shared_sum = call(
        shared_kernel, array(tok, 2 * hid_s + LANES), [vmem()] * 4
    )(mixed, gain, shared_gate, shared_up)

    def add(a, b, width):
        return call(functools.partial(add_kernel, width=width), array(*a.shape), [vmem()] * 2)(a, b)

    def hidden(a, b, width):
        return call(
            functools.partial(hidden_kernel, width=width, features=features),
            array(a.shape[0], width // 2),
            [vmem()] * 2,
        )(a, b)

    for bit in bits[:-1]:
        shared_sum = add(shared_sum, swap(shared_sum, "tp", bit), 2 * hid_s)
    other = swap(shared_sum, "tp", bits[-1])
    shared_hidden = hidden(shared_sum, other, 2 * hid_s)

    width = 2 * gate_proj.shape[2]
    weights = [gain, gate_proj, up_proj] + others[:3]
    back = {}
    for ms in groups:
        total = call(
            routed_kernel, array(len(ms) * cap, width + LANES), [smem()] + [vmem()] * (len(ms) + 6)
        )(at, *[arrived[m] for m in ms], *weights)
        for bit in bits[1:-1]:
            total = add(total, swap(total, "tp", bit), width)
        came = swap(total, "tp", bits[-1])
        outs = call(
            functools.partial(down_kernel, width=width, features=features),
            (array(2, cap, feats),) * len(ms),
            [smem()] + [vmem()] * 4,
        )(at, total, came, down_proj, others[3])
        for m, out in zip(ms, outs):
            back[m] = swap(out, "sp", m)
    total, *picks = call(
        functools.partial(base_kernel, local=local, cap=cap),
        (jax.ShapeDtypeStruct((2, tok, feats), F32),)
        + tuple(array(tok, 2 * len(ms) * cap) for ms in groups),
        [smem()] + [vmem()] * 5,
    )(at, expert_ids.T, route_weights.T, mixed, shared_hidden, shared_down)
    for i in (1, 0, 2):
        ms, last = groups[i], i == 2
        one = jax.ShapeDtypeStruct((tok, feats), F32)
        total = call(
            functools.partial(combine_kernel, outs=2 if last else 1),
            (one, one) if last else jax.ShapeDtypeStruct((2, tok, feats), F32),
            [vmem()] * (2 + len(ms)),
        )(total, picks[i], *[back[m] for m in ms])
    return call(final_kernel, array(tok, feats), [vmem()] * 2)(total[0], swap(total[1], "tp", 1))


def solution(mesh):
    in_specs = (
        P("sp", "tp"),
        P("sp", "tp"),
        P("sp", "tp"),
        P("sp", "tp"),
        P("sp", "tp"),
        P(None, "tp"),
        P("tp"),
        P("sp", None),
        P("sp", None),
        P("sp", "tp", None),
        P("sp", "tp", None),
        P("sp", None, "tp"),
        P("tp", None),
        P("tp", None),
        P(None, "tp"),
    )
    out_specs = P("sp", "tp")
    return jax.shard_map(layer, mesh=mesh, in_specs=in_specs, out_specs=out_specs, check_vma=False)
```

```python
import functools

import jax
import jax.numpy as jnp
from jax import lax
from jax.experimental import pallas as pl
from jax.experimental.pallas import tpu as pltpu
from jax.sharding import PartitionSpec as P


EPS = 1e-06
LANES = 128
BIAS_ROWS = 16
VMEM_LIMIT = 16 * 1024 * 1024
BF = jnp.bfloat16
F32 = jnp.float32


def vmem():
    return pl.BlockSpec(memory_space=pltpu.VMEM)


def hbm():
    return pl.BlockSpec(memory_space=pltpu.HBM)


def in_hbm(x):
    return pltpu.with_memory_space_constraint(x, pltpu.HBM)


def smem():
    return pl.BlockSpec(memory_space=pltpu.SMEM)


def call(kernel, out_shape, in_specs, scratch=()):
    many = isinstance(out_shape, (tuple, list))
    return pl.pallas_call(
        kernel,
        out_shape=out_shape,
        in_specs=in_specs,
        out_specs=tuple(vmem() for _ in out_shape) if many else vmem(),
        scratch_shapes=list(scratch),
        compiler_params=pltpu.CompilerParams(vmem_limit_bytes=VMEM_LIMIT),
    )


def iota(shape, dim):
    return lax.broadcasted_iota(jnp.int32, shape, dim)


def dot(a, b):
    return jnp.dot(a, b, preferred_element_type=F32)


def split_pair(x):
    high = x.astype(BF)
    return high, (x - high.astype(F32)).astype(BF)


def pack_kernel(at_ref, q_ref, k_ref, v_ref, b_ref, *refs, hd):
    heads = (len(refs) - 2) // 2
    outs, queries, bias_ref, sems = refs[:heads], refs[heads:-2], refs[-2], refs[-1]
    tok = k_ref.shape[0]
    fetch = pltpu.make_async_copy(b_ref, bias_ref, sems.at[3 * heads])
    fetch.start()
    copies = []
    for mh, out in enumerate(outs):
        head = jnp.bitwise_xor(at_ref[0], mh)
        cols = pl.ds(pl.multiple_of(head * hd, hd), hd)
        for i, (src, target) in enumerate(
            (
                (k_ref, out.at[pl.ds(0, tok)]),
                (v_ref, out.at[pl.ds(tok, tok)]),
                (q_ref, queries[mh]),
            )
        ):
            copy = pltpu.make_async_copy(src.at[:, cols], target, sems.at[3 * mh + i])
            copy.start()
            copies.append(copy)
    fetch.wait()
    bias = bias_ref[...].astype(F32)
    for mh, out in enumerate(outs):
        head = jnp.bitwise_xor(at_ref[0], mh)
        row = jnp.where(iota(bias.shape, 0) == head, bias, 0.0)
        row = jnp.sum(row, axis=0, keepdims=True)
        out[2 * tok : 2 * tok + BIAS_ROWS] = jnp.broadcast_to(row, (BIAS_ROWS, tok)).astype(BF)
    for copy in copies:
        copy.wait()


def lay_kernel(at_ref, *refs):
    for i, (ref, out) in enumerate(zip(refs[:4], refs[4:5] * 2 + refs[5:6] * 2)):
        value = ref[at_ref[4]] if i < 2 else ref[...]
        width = value.shape[1]
        out[:, i % 2 * width : (i % 2 + 1) * width] = value


def attention_kernel(at_ref, *refs, heads, group):
    blocks = heads * group
    weights, refs = refs[:5], refs[5:]
    ins, q_ins, outs = refs[:blocks], refs[blocks : blocks + heads], refs[blocks + heads : -8]
    w_ref, laid_ref, shared_ref, kv_ref, q_ref, acc_ref, carry_ref, sems = refs[-8:]
    e = at_ref[4]
    moves = [(weights[0], w_ref)]
    for i, src in enumerate((weights[1].at[e], weights[2].at[e], *weights[3:])):
        cols = pl.ds(i % 2 * src.shape[1], src.shape[1])
        moves.append((src, (laid_ref if i < 2 else shared_ref).at[:, cols]))
    fetches = [pltpu.make_async_copy(a, b, sems.at[i]) for i, (a, b) in enumerate(moves)]
    for fetch in fetches:
        fetch.start()
    tok, hd = q_ins[0].shape
    h, p = at_ref[0], at_ref[1]
    for mh in range(heads):
        g = jnp.bitwise_xor(h, mh)
        q_ref[pl.ds(pl.multiple_of(g * tok, tok), tok)] = q_ins[mh][...]
        for mp in range(group):
            kv_ref[g * group + jnp.bitwise_xor(p, mp)] = ins[mh * group + mp][...]
    acc_ref[...] = jnp.zeros_like(acc_ref)
    carry_ref[...] = jnp.zeros_like(carry_ref)
    span = 2 if group % 2 == 0 else 1
    keys_all = span * tok
    tri = jnp.where(
        iota((keys_all, keys_all), 0) > iota((keys_all, keys_all), 1), 1.0, 0.0
    ).astype(BF)
    scale = hd ** (-0.5)

    def pair(j, start, stop, axis=0):
        return jnp.concatenate([kv_ref[j + i, start:stop] for i in range(span)], axis=axis)

    for j in reversed(range(0, blocks, span)):
        r0 = (j // group) * tok
        n = heads * tok - r0
        keys, values = pair(j, 0, tok), pair(j, tok, 2 * tok)
        bias = pair(j, 2 * tok, 2 * tok + BIAS_ROWS, 1).astype(F32)[0:1, :]
        raw = lax.dot_general(
            q_ref[r0:], keys, (((1,), (1,)), ((), ())), preferred_element_type=F32
        )
        logits = raw * scale + bias
        soft = jnp.log(1.0 + jnp.exp(-jnp.abs(logits)))
        stay = jnp.minimum(logits, 0.0) - soft
        loss = jnp.maximum(logits, 0.0) + soft
        before = iota((tok, keys_all), 1) < iota((tok, keys_all), 0) + (p - j % group) * tok

        def masked(x):
            first = jnp.where(before, x[:tok], 0.0)
            return jnp.concatenate([first, x[tok:]], axis=0) if n > tok else first

        loss = masked(loss)
        sums = dot(jnp.concatenate(split_pair(loss), axis=0), tri)
        sums = sums[:n] + sums[n:]
        carry = carry_ref[r0:]
        later = sums + jnp.concatenate([carry] * span, axis=1)
        weights = masked(jnp.exp(stay - later))
        carry_ref[r0:] = carry + (sums[:, 0:1] + loss[:, 0:1])
        acc_ref[r0:] += dot(weights.astype(BF), values)
    for mh in range(heads):
        g = jnp.bitwise_xor(h, mh)
        outs[mh][...] = acc_ref[pl.ds(pl.multiple_of(g * tok, tok), tok)].astype(BF)
    for fetch in fetches:
        fetch.wait()


def stack_kernel(*refs):
    for i, ref in enumerate(refs[:-1]):
        refs[-1][i] = ref[...]


def slots_of(ids_ref, s, c, local, blocks):
    tok = ids_ref.shape[1]
    expert = jnp.bitwise_xor(iota((blocks, tok), 0), s) * local + c
    named = [expert == ids_ref[k : k + 1, :] for k in range(ids_ref.shape[0])]
    hit = functools.reduce(jnp.logical_or, named)
    order = jnp.where(iota((tok, tok), 0) < iota((tok, tok), 1), 1.0, 0.0).astype(BF)
    rank = dot(jnp.where(hit, 1.0, 0.0).astype(BF), order)
    return named, jnp.where(hit, rank, -1.0)


def spread(rank, values, cap):
    slot = iota((cap, rank.shape[1]), 0).astype(F32)
    return jnp.concatenate(
        [
            jnp.where(slot == rank[e : e + 1, :], values[e : e + 1, :], 0.0)
            for e in range(rank.shape[0])
        ],
        axis=0,
    )


def project_kernel(at_ref, *refs, masks, heads):
    count = len(masks)
    pieces = refs[:count]
    w_ref, stream_ref, mixed_ref, rows_ref = refs[count:]
    h, t = at_ref[0], at_ref[2]
    for mask, piece in zip(masks, pieces):
        hd = piece.shape[2]
        for mh in range(heads):
            head = jnp.bitwise_xor(t, mask) * heads + jnp.bitwise_xor(h, mh)
            rows_ref[:, pl.ds(pl.multiple_of(head * hd, hd), hd)] = piece[mh]
    total = stream_ref[...].astype(F32) + dot(rows_ref[...], w_ref[...])
    mixed_ref[...] = total.astype(BF)


def dispatch_kernel(at_ref, ids_ref, own_ref, other_ref, *sends, local):
    cap = sends[0].shape[1]
    _, rank = slots_of(ids_ref, at_ref[3], at_ref[4], local, len(sends))
    pick = spread(rank, jnp.ones_like(rank), cap).astype(BF)
    for side, ref in enumerate((own_ref, other_ref)):
        rows = dot(pick, ref[...]).astype(BF)
        for m, send in enumerate(sends):
            send[side] = rows[m * cap : (m + 1) * cap]


def square_lanes(square):
    high, low = split_pair(square)
    lane = iota((square.shape[0], LANES), 1)
    tail = jnp.where(lane == 0, high.astype(F32), jnp.where(lane == 1, low.astype(F32), 0.0))
    return tail.astype(BF)


def weighted(xs, gain_refs, w_refs):
    total, square = 0.0, 0.0
    for x, gain_ref, w_ref in zip(xs, gain_refs, w_refs):
        square = square + jnp.sum(x * x, axis=1, keepdims=True)
        scaled = (x * gain_ref[...]).astype(BF)
        total = total + dot(scaled, w_ref[...]).astype(BF).astype(F32)
    return jnp.concatenate([total.astype(BF), square_lanes(square)], axis=1)


def shared_kernel(at_ref, own_ref, other_ref, *refs):
    out_ref = refs[-1]
    count = out_ref.shape[0]
    part = pl.ds(pl.multiple_of(at_ref[4] * count, count), count)
    xs = [ref[part].astype(F32) for ref in (own_ref, other_ref)]
    out_ref[...] = weighted(xs, refs[:2], refs[2:4])


def routed_kernel(*refs):
    xs = [
        jnp.concatenate([ref[side].astype(F32) for ref in refs[4:-1]], axis=0)
        for side in range(2)
    ]
    refs[-1][...] = weighted(xs, refs[:2], refs[2:4])


def add_partials(a_ref, b_ref, width):
    a = a_ref[...].astype(F32)
    b = b_ref[...].astype(F32)
    body = a[:, :width] + b[:, :width]
    square = a[:, width : width + 1] + b[:, width : width + 1]
    square = square + (a[:, width + 1 : width + 2] + b[:, width + 1 : width + 2])
    return body, square


def add_kernel(a_ref, b_ref, out_ref, *, width):
    body, square = add_partials(a_ref, b_ref, width)
    out_ref[...] = jnp.concatenate([body.astype(BF), square_lanes(square)], axis=1)


def hidden_of(a_ref, b_ref, width, features):
    body, square = add_partials(a_ref, b_ref, width)
    inv = lax.rsqrt(square / features + EPS)
    gate = body[:, : width // 2] * inv
    up = body[:, width // 2 :] * inv
    return (gate * jax.nn.sigmoid(gate) * up).astype(BF)


def hidden_kernel(a_ref, b_ref, out_ref, *, width, features):
    out_ref[...] = hidden_of(a_ref, b_ref, width, features)


def down_kernel(at_ref, a_ref, b_ref, own_ref, other_ref, *outs, width, features):
    hidden = hidden_of(a_ref, b_ref, width, features)
    cap = outs[0].shape[1]
    for side, w_ref in enumerate((own_ref, other_ref)):
        rows = dot(hidden, w_ref[at_ref[4]]).astype(BF)
        for i, out in enumerate(outs):
            out[side] = rows[i * cap : (i + 1) * cap]


def base_kernel(
    at_ref, ids_ref, rw_ref, mixed_ref, mine_ref, theirs_ref, down_ref, base_ref, *picks, local, cap
):
    blocks = sum(pick.shape[1] for pick in picks) // (2 * cap)
    named, rank = slots_of(ids_ref, at_ref[3], at_ref[4], local, blocks)
    weight = functools.reduce(
        jnp.add,
        [jnp.where(hit, rw_ref[k : k + 1, :], 0.0) for k, hit in enumerate(named)],
    )
    high, low = split_pair(jnp.transpose(spread(rank, weight, cap)))
    start = 0
    for pick in picks:
        width = pick.shape[1] // 2
        pick[:, :width] = high[:, start : start + width]
        pick[:, width:] = low[:, start : start + width]
        start += width
    first = at_ref[4] == 0
    mine, theirs = mine_ref[...].astype(F32), theirs_ref[...].astype(F32)
    hid = [jnp.where(first, mine, theirs), jnp.where(first, theirs, mine)]
    hid = jnp.concatenate(hid, axis=0).astype(BF)
    base_ref[0] = mixed_ref[...].astype(F32) + dot(hid, down_ref[...])
    base_ref[1] = jnp.zeros_like(base_ref[1])


def combine_kernel(base_ref, pick_ref, *refs, outs):
    backs, out_refs = refs[:-outs], refs[-outs:]
    for side in range(2):
        rows = jnp.concatenate([ref[side] for ref in backs], axis=0)
        rows = jnp.concatenate([rows, rows], axis=0)
        total = base_ref[side] + dot(pick_ref[...], rows)
        if outs == 1:
            out_refs[0][side] = total
        else:
            out_refs[side][...] = total


def final_kernel(a_ref, b_ref, out_ref):
    out_ref[...] = (a_ref[...] + b_ref[...]).astype(BF)


def swap(x, axis, bit):
    if bit == 0:
        return x
    count = lax.axis_size(axis)
    return lax.ppermute(x, axis, [(i, i ^ bit) for i in range(count)])


def layer(
    queries,
    key_rows,
    value_rows,
    break_bias,
    stream,
    out_proj,
    norm_gain,
    expert_ids,
    route_weights,
    gate_proj,
    up_proj,
    down_proj,
    shared_gate,
    shared_up,
    shared_down,
):
    tok = queries.shape[0]
    heads = break_bias.shape[1]
    hd = queries.shape[1] // heads
    blocks = lax.axis_size("sp")
    tp = lax.axis_size("tp")
    feats = stream.shape[1]
    features = feats * tp
    s_index = lax.axis_index("sp").astype(jnp.int32)
    t_index = lax.axis_index("tp").astype(jnp.int32)
    group = blocks // heads
    h_index, p_index = s_index // group, s_index % group

    def array(*shape):
        return jax.ShapeDtypeStruct(shape, BF)

    at = jnp.stack([h_index, p_index, t_index, s_index, t_index % 2])
    kv_rows = 2 * tok + BIAS_ROWS
    gain = norm_gain.reshape(1, feats)
    others = [
        swap(x, "tp", 1)
        for x in (gain, gate_proj, up_proj, shared_gate, shared_up, down_proj)
    ]
    packed = call(
        functools.partial(pack_kernel, hd=hd),
        (array(kv_rows, hd),) * heads + (array(tok, hd),) * heads,
        [smem()] + [hbm()] * 4,
        [pltpu.VMEM((heads, tok), BF), pltpu.SemaphoreType.DMA((3 * heads + 1,))],
    )(at, *[in_hbm(x) for x in (queries, key_rows, value_rows, break_bias.T)])
    kv = [swap(packed[mh], "sp", mh * group) for mh in range(heads)]
    kv = [swap(kv[mh], "sp", mp) for mh in range(heads) for mp in range(group)]
    q = [swap(packed[heads + mh], "sp", mh * group) for mh in range(heads)]
    hid_s = shared_gate.shape[1]
    width = 2 * gate_proj.shape[2]
    wide = (array(feats, width), array(feats, 2 * hid_s))
    laid_other, shared_other = call(lay_kernel, wide, [smem()] + [vmem()] * 4)(at, *others[1:5])
    *attended, out_w, laid_own, shared_own = call(
        functools.partial(attention_kernel, heads=heads, group=group),
        (array(tok, hd),) * heads + (array(*out_proj.shape),) + wide,
        [smem()] + [hbm()] * 5 + [vmem()] * (blocks + heads),
        [
            pltpu.VMEM((blocks, kv_rows, hd), BF),
            pltpu.VMEM((heads * tok, hd), BF),
            pltpu.VMEM((heads * tok, hd), F32),
            pltpu.VMEM((heads * tok, tok), F32),
            pltpu.SemaphoreType.DMA((5,)),
        ],
    )(
        at,
        *[in_hbm(x) for x in (out_proj, gate_proj, up_proj, shared_gate, shared_up)],
        *kv,
        *q,
    )
    piece = call(stack_kernel, array(heads, tok, hd), [vmem()] * heads)(
        *[swap(attended[mh], "sp", mh * group) for mh in range(heads)]
    )
    bits = [1 << i for i in range(tp.bit_length() - 1)]
    pieces, masks = [piece], [0]
    for bit in reversed(bits):
        pieces = pieces + [swap(x, "tp", bit) for x in pieces]
        masks = masks + [m ^ bit for m in masks]

    local = gate_proj.shape[0]
    experts = local * blocks
    choices = expert_ids.shape[1]
    cap = 2 * choices * tok // experts
    mixed = call(
        functools.partial(project_kernel, masks=tuple(masks), heads=heads),
        array(tok, feats),
        [smem()] + [vmem()] * (len(pieces) + 2),
        [pltpu.VMEM((tok, out_proj.shape[0]), BF)],
    )(at, *pieces, out_w, stream)
    mixed_other = swap(mixed, "tp", 1)
    sends = call(
        functools.partial(dispatch_kernel, local=local),
        (array(2, cap, feats),) * blocks,
        [smem()] + [vmem()] * 3,
    )(at, expert_ids.T, mixed, mixed_other)

    half = blocks // 2
    quarter = half + half // 2
    groups = [range(half), range(half, quarter), range(quarter, blocks)]
    arrived = {m: swap(sends[m], "sp", m) for m in range(blocks)}

    shared_sum = call(
        shared_kernel, array(tok // 2, 2 * hid_s + LANES), [smem()] + [vmem()] * 6
    )(at, mixed, mixed_other, gain, others[0], shared_own, shared_other)

    def add(a, b, width):
        return call(functools.partial(add_kernel, width=width), array(*a.shape), [vmem()] * 2)(a, b)

    def hidden(a, b, width):
        return call(
            functools.partial(hidden_kernel, width=width, features=features),
            array(a.shape[0], width // 2),
            [vmem()] * 2,
        )(a, b)

    for bit in bits[1:-1]:
        other = swap(shared_sum, "tp", bit)
        shared_sum = add(shared_sum, other, 2 * hid_s)
    other = swap(shared_sum, "tp", bits[-1])
    shared_hidden = hidden(shared_sum, other, 2 * hid_s)
    other_hidden = swap(shared_hidden, "tp", 1)

    back = {}
    for ms in groups:
        total = call(
            routed_kernel, array(len(ms) * cap, width + LANES), [vmem()] * (len(ms) + 4)
        )(gain, others[0], laid_own, laid_other, *[arrived[m] for m in ms])
        for bit in bits[1:-1]:
            total = add(total, swap(total, "tp", bit), width)
        came = swap(total, "tp", bits[-1])
        outs = call(
            functools.partial(down_kernel, width=width, features=features),
            (array(2, cap, feats),) * len(ms),
            [smem()] + [vmem()] * 4,
        )(at, total, came, down_proj, others[5])
        for m, out in zip(ms, outs):
            back[m] = swap(out, "sp", m)
    total, *picks = call(
        functools.partial(base_kernel, local=local, cap=cap),
        (jax.ShapeDtypeStruct((2, tok, feats), F32),)
        + tuple(array(tok, 2 * len(ms) * cap) for ms in groups),
        [smem()] + [vmem()] * 6,
    )(at, expert_ids.T, route_weights.T, mixed, shared_hidden, other_hidden, shared_down)
    for i in (1, 0, 2):
        ms, last = groups[i], i == 2
        one = jax.ShapeDtypeStruct((tok, feats), F32)
        total = call(
            functools.partial(combine_kernel, outs=2 if last else 1),
            (one, one) if last else jax.ShapeDtypeStruct((2, tok, feats), F32),
            [vmem()] * (2 + len(ms)),
        )(total, picks[i], *[back[m] for m in ms])
    return call(final_kernel, array(tok, feats), [vmem()] * 2)(total[0], swap(total[1], "tp", 1))


def solution(mesh):
    in_specs = (
        P("sp", "tp"),
        P("sp", "tp"),
        P("sp", "tp"),
        P("sp", "tp"),
        P("sp", "tp"),
        P(None, "tp"),
        P("tp"),
        P("sp", None),
        P("sp", None),
        P("sp", "tp", None),
        P("sp", "tp", None),
        P("sp", None, "tp"),
        P("tp", None),
        P("tp", None),
        P(None, "tp"),
    )
    out_specs = P("sp", "tp")
    return jax.shard_map(layer, mesh=mesh, in_specs=in_specs, out_specs=out_specs, check_vma=False)
```

```python
import functools

import jax
import jax.numpy as jnp
from jax import lax
from jax.experimental import pallas as pl
from jax.experimental.pallas import tpu as pltpu
from jax.sharding import PartitionSpec as P


EPS = 1e-06
LANES = 128
BIAS_ROWS = 16
VMEM_LIMIT = 16 * 1024 * 1024
BF = jnp.bfloat16
F32 = jnp.float32


def vmem():
    return pl.BlockSpec(memory_space=pltpu.VMEM)


def hbm():
    return pl.BlockSpec(memory_space=pltpu.HBM)


def in_hbm(x):
    return pltpu.with_memory_space_constraint(x, pltpu.HBM)


def smem():
    return pl.BlockSpec(memory_space=pltpu.SMEM)


def call(kernel, out_shape, in_specs, scratch=()):
    many = isinstance(out_shape, (tuple, list))
    return pl.pallas_call(
        kernel,
        out_shape=out_shape,
        in_specs=in_specs,
        out_specs=tuple(vmem() for _ in out_shape) if many else vmem(),
        scratch_shapes=list(scratch),
        compiler_params=pltpu.CompilerParams(vmem_limit_bytes=VMEM_LIMIT),
    )


def iota(shape, dim):
    return lax.broadcasted_iota(jnp.int32, shape, dim)


def dot(a, b):
    return jnp.dot(a, b, preferred_element_type=F32)


def split_pair(x):
    high = x.astype(BF)
    return high, (x - high.astype(F32)).astype(BF)


def pack_kernel(at_ref, q_ref, k_ref, v_ref, b_ref, *refs, hd):
    heads = (len(refs) - 2) // 2
    outs, queries, bias_ref, sems = refs[:heads], refs[heads:-2], refs[-2], refs[-1]
    tok = k_ref.shape[0]
    fetch = pltpu.make_async_copy(b_ref, bias_ref, sems.at[3 * heads])
    fetch.start()
    copies = []
    for mh, out in enumerate(outs):
        head = jnp.bitwise_xor(at_ref[0], mh)
        cols = pl.ds(pl.multiple_of(head * hd, hd), hd)
        for i, (src, target) in enumerate(
            (
                (k_ref, out.at[pl.ds(0, tok)]),
                (v_ref, out.at[pl.ds(tok, tok)]),
                (q_ref, queries[mh]),
            )
        ):
            copy = pltpu.make_async_copy(src.at[:, cols], target, sems.at[3 * mh + i])
            copy.start()
            copies.append(copy)
    fetch.wait()
    bias = bias_ref[...].astype(F32)
    for mh, out in enumerate(outs):
        head = jnp.bitwise_xor(at_ref[0], mh)
        row = jnp.where(iota(bias.shape, 0) == head, bias, 0.0)
        row = jnp.sum(row, axis=0, keepdims=True)
        out[2 * tok : 2 * tok + BIAS_ROWS] = jnp.broadcast_to(row, (BIAS_ROWS, tok)).astype(BF)
    for copy in copies:
        copy.wait()


def lay_kernel(at_ref, own_gate, own_up, *refs):
    own_ref, sems = refs[6:]
    copies = []
    for i, src in enumerate((own_gate, own_up)):
        cols = pl.ds(i * src.shape[1], src.shape[1])
        copies.append(pltpu.make_async_copy(src, own_ref.at[:, cols], sems.at[i]))
        copies[-1].start()
    for i, (ref, out) in enumerate(zip(refs[:4], refs[4:5] * 2 + refs[5:6] * 2)):
        value = ref[at_ref[4]] if i < 2 else ref[...]
        width = value.shape[1]
        out[:, i % 2 * width : (i % 2 + 1) * width] = value
    for copy in copies:
        copy.wait()


def attention_kernel(at_ref, *refs, heads, group):
    blocks = heads * group
    weights, refs = refs[:3], refs[3:]
    ins, q_ins, outs = refs[:blocks], refs[blocks : blocks + heads], refs[blocks + heads : -7]
    w_ref, laid_ref, kv_ref, q_ref, acc_ref, carry_ref, sems = refs[-7:]
    e = at_ref[4]
    moves = [(weights[0], w_ref)]
    for i, src in enumerate((weights[1].at[e], weights[2].at[e])):
        cols = pl.ds(i * src.shape[1], src.shape[1])
        moves.append((src, laid_ref.at[:, cols]))
    fetches = [pltpu.make_async_copy(a, b, sems.at[i]) for i, (a, b) in enumerate(moves)]
    for fetch in fetches:
        fetch.start()
    tok, hd = q_ins[0].shape
    h, p = at_ref[0], at_ref[1]
    for mh in range(heads):
        g = jnp.bitwise_xor(h, mh)
        q_ref[pl.ds(pl.multiple_of(g * tok, tok), tok)] = q_ins[mh][...]
        for mp in range(group):
            kv_ref[g * group + jnp.bitwise_xor(p, mp)] = ins[mh * group + mp][...]
    acc_ref[...] = jnp.zeros_like(acc_ref)
    carry_ref[...] = jnp.zeros_like(carry_ref)
    span = 2 if group % 2 == 0 else 1
    keys_all = span * tok
    tri = jnp.where(
        iota((keys_all, keys_all), 0) > iota((keys_all, keys_all), 1), 1.0, 0.0
    ).astype(BF)
    scale = hd ** (-0.5)

    def pair(j, start, stop, axis=0):
        return jnp.concatenate([kv_ref[j + i, start:stop] for i in range(span)], axis=axis)

    for j in reversed(range(0, blocks, span)):
        r0 = (j // group) * tok
        n = heads * tok - r0
        keys, values = pair(j, 0, tok), pair(j, tok, 2 * tok)
        bias = pair(j, 2 * tok, 2 * tok + BIAS_ROWS, 1).astype(F32)[0:1, :]
        raw = lax.dot_general(
            q_ref[r0:], keys, (((1,), (1,)), ((), ())), preferred_element_type=F32
        )
        logits = raw * scale + bias
        soft = jnp.log(1.0 + jnp.exp(-jnp.abs(logits)))
        stay = jnp.minimum(logits, 0.0) - soft
        loss = jnp.maximum(logits, 0.0) + soft
        before = iota((tok, keys_all), 1) < iota((tok, keys_all), 0) + (p - j % group) * tok

        def masked(x):
            first = jnp.where(before, x[:tok], 0.0)
            return jnp.concatenate([first, x[tok:]], axis=0) if n > tok else first

        loss = masked(loss)
        sums = dot(jnp.concatenate(split_pair(loss), axis=0), tri)
        sums = sums[:n] + sums[n:]
        carry = carry_ref[r0:]
        later = sums + jnp.concatenate([carry] * span, axis=1)
        weights = masked(jnp.exp(stay - later))
        carry_ref[r0:] = carry + (sums[:, 0:1] + loss[:, 0:1])
        acc_ref[r0:] += dot(weights.astype(BF), values)
    for mh in range(heads):
        g = jnp.bitwise_xor(h, mh)
        outs[mh][...] = acc_ref[pl.ds(pl.multiple_of(g * tok, tok), tok)].astype(BF)
    for fetch in fetches:
        fetch.wait()


def stack_kernel(*refs):
    for i, ref in enumerate(refs[:-1]):
        refs[-1][i] = ref[...]


def slots_of(ids_ref, s, c, local, blocks):
    tok = ids_ref.shape[1]
    expert = jnp.bitwise_xor(iota((blocks, tok), 0), s) * local + c
    named = [expert == ids_ref[k : k + 1, :] for k in range(ids_ref.shape[0])]
    hit = functools.reduce(jnp.logical_or, named)
    order = jnp.where(iota((tok, tok), 0) < iota((tok, tok), 1), 1.0, 0.0).astype(BF)
    rank = dot(jnp.where(hit, 1.0, 0.0).astype(BF), order)
    return named, jnp.where(hit, rank, -1.0)


def spread(rank, values, cap):
    slot = iota((cap, rank.shape[1]), 0).astype(F32)
    return jnp.concatenate(
        [
            jnp.where(slot == rank[e : e + 1, :], values[e : e + 1, :], 0.0)
            for e in range(rank.shape[0])
        ],
        axis=0,
    )


def project_kernel(at_ref, *refs, masks, heads):
    count = len(masks)
    pieces = refs[:count]
    w_ref, stream_ref, mixed_ref, rows_ref = refs[count:]
    h, t = at_ref[0], at_ref[2]
    for mask, piece in zip(masks, pieces):
        hd = piece.shape[2]
        for mh in range(heads):
            head = jnp.bitwise_xor(t, mask) * heads + jnp.bitwise_xor(h, mh)
            rows_ref[:, pl.ds(pl.multiple_of(head * hd, hd), hd)] = piece[mh]
    total = stream_ref[...].astype(F32) + dot(rows_ref[...], w_ref[...])
    mixed_ref[...] = total.astype(BF)


def dispatch_kernel(at_ref, ids_ref, own_ref, other_ref, *sends, local):
    cap = sends[0].shape[1]
    _, rank = slots_of(ids_ref, at_ref[3], at_ref[4], local, len(sends))
    pick = spread(rank, jnp.ones_like(rank), cap).astype(BF)
    for side, ref in enumerate((own_ref, other_ref)):
        rows = dot(pick, ref[...]).astype(BF)
        for m, send in enumerate(sends):
            send[side] = rows[m * cap : (m + 1) * cap]


def square_lanes(square):
    high, low = split_pair(square)
    lane = iota((square.shape[0], LANES), 1)
    tail = jnp.where(lane == 0, high.astype(F32), jnp.where(lane == 1, low.astype(F32), 0.0))
    return tail.astype(BF)


def weighted(xs, gain_refs, w_refs):
    total, square = 0.0, 0.0
    for x, gain_ref, w_ref in zip(xs, gain_refs, w_refs):
        square = square + jnp.sum(x * x, axis=1, keepdims=True)
        scaled = (x * gain_ref[...]).astype(BF)
        total = total + dot(scaled, w_ref[...]).astype(BF).astype(F32)
    return jnp.concatenate([total.astype(BF), square_lanes(square)], axis=1)


def shared_kernel(at_ref, own_ref, other_ref, *refs):
    out_ref = refs[-1]
    count = out_ref.shape[0]
    part = pl.ds(pl.multiple_of(at_ref[4] * count, count), count)
    xs = [ref[part].astype(F32) for ref in (own_ref, other_ref)]
    out_ref[...] = weighted(xs, refs[:2], refs[2:4])


def routed_kernel(*refs):
    xs = [
        jnp.concatenate([ref[side].astype(F32) for ref in refs[4:-1]], axis=0)
        for side in range(2)
    ]
    refs[-1][...] = weighted(xs, refs[:2], refs[2:4])


def add_partials(a_ref, b_ref, width):
    a = a_ref[...].astype(F32)
    b = b_ref[...].astype(F32)
    body = a[:, :width] + b[:, :width]
    square = a[:, width : width + 1] + b[:, width : width + 1]
    square = square + (a[:, width + 1 : width + 2] + b[:, width + 1 : width + 2])
    return body, square


def add_kernel(a_ref, b_ref, out_ref, *, width):
    body, square = add_partials(a_ref, b_ref, width)
    out_ref[...] = jnp.concatenate([body.astype(BF), square_lanes(square)], axis=1)


def hidden_of(a_ref, b_ref, width, features):
    body, square = add_partials(a_ref, b_ref, width)
    inv = lax.rsqrt(square / features + EPS)
    gate = body[:, : width // 2] * inv
    up = body[:, width // 2 :] * inv
    return (gate * jax.nn.sigmoid(gate) * up).astype(BF)


def hidden_kernel(a_ref, b_ref, out_ref, *, width, features):
    out_ref[...] = hidden_of(a_ref, b_ref, width, features)


def down_kernel(at_ref, a_ref, b_ref, own_ref, other_ref, *outs, width, features):
    hidden = hidden_of(a_ref, b_ref, width, features)
    cap = outs[0].shape[1]
    for side, w_ref in enumerate((own_ref, other_ref)):
        rows = dot(hidden, w_ref[at_ref[4]]).astype(BF)
        for i, out in enumerate(outs):
            out[side] = rows[i * cap : (i + 1) * cap]


def base_kernel(
    at_ref, ids_ref, rw_ref, mixed_ref, mine_ref, theirs_ref, down_ref, base_ref, *picks, local, cap
):
    blocks = sum(pick.shape[1] for pick in picks) // (2 * cap)
    named, rank = slots_of(ids_ref, at_ref[3], at_ref[4], local, blocks)
    weight = functools.reduce(
        jnp.add,
        [jnp.where(hit, rw_ref[k : k + 1, :], 0.0) for k, hit in enumerate(named)],
    )
    high, low = split_pair(jnp.transpose(spread(rank, weight, cap)))
    start = 0
    for pick in picks:
        width = pick.shape[1] // 2
        pick[:, :width] = high[:, start : start + width]
        pick[:, width:] = low[:, start : start + width]
        start += width
    first = at_ref[4] == 0
    mine, theirs = mine_ref[...].astype(F32), theirs_ref[...].astype(F32)
    hid = [jnp.where(first, mine, theirs), jnp.where(first, theirs, mine)]
    hid = jnp.concatenate(hid, axis=0).astype(BF)
    base_ref[0] = mixed_ref[...].astype(F32) + dot(hid, down_ref[...])
    base_ref[1] = jnp.zeros_like(base_ref[1])


def combine_kernel(base_ref, pick_ref, *refs, outs):
    backs, out_refs = refs[:-outs], refs[-outs:]
    for side in range(2):
        rows = jnp.concatenate([ref[side] for ref in backs], axis=0)
        rows = jnp.concatenate([rows, rows], axis=0)
        total = base_ref[side] + dot(pick_ref[...], rows)
        if outs == 1:
            out_refs[0][side] = total
        else:
            out_refs[side][...] = total.astype(out_refs[side].dtype)


def final_kernel(a_ref, b_ref, out_ref):
    out_ref[...] = (a_ref[...] + b_ref[...].astype(F32)).astype(BF)


def swap(x, axis, bit):
    if bit == 0:
        return x
    count = lax.axis_size(axis)
    return lax.ppermute(x, axis, [(i, i ^ bit) for i in range(count)])


def layer(
    queries,
    key_rows,
    value_rows,
    break_bias,
    stream,
    out_proj,
    norm_gain,
    expert_ids,
    route_weights,
    gate_proj,
    up_proj,
    down_proj,
    shared_gate,
    shared_up,
    shared_down,
):
    tok = queries.shape[0]
    heads = break_bias.shape[1]
    hd = queries.shape[1] // heads
    blocks = lax.axis_size("sp")
    tp = lax.axis_size("tp")
    feats = stream.shape[1]
    features = feats * tp
    s_index = lax.axis_index("sp").astype(jnp.int32)
    t_index = lax.axis_index("tp").astype(jnp.int32)
    group = blocks // heads
    h_index, p_index = s_index // group, s_index % group

    def array(*shape):
        return jax.ShapeDtypeStruct(shape, BF)

    at = jnp.stack([h_index, p_index, t_index, s_index, t_index % 2])
    kv_rows = 2 * tok + BIAS_ROWS
    gain = norm_gain.reshape(1, feats)
    others = [
        swap(x, "tp", 1)
        for x in (gain, gate_proj, up_proj, shared_gate, shared_up, down_proj)
    ]
    packed = call(
        functools.partial(pack_kernel, hd=hd),
        (array(kv_rows, hd),) * heads + (array(tok, hd),) * heads,
        [smem()] + [hbm()] * 4,
        [pltpu.VMEM((heads, tok), BF), pltpu.SemaphoreType.DMA((3 * heads + 1,))],
    )(at, *[in_hbm(x) for x in (queries, key_rows, value_rows, break_bias.T)])
    kv = [swap(packed[mh], "sp", mh * group) for mh in range(heads)]
    kv = [swap(kv[mh], "sp", mp) for mh in range(heads) for mp in range(group)]
    q = [swap(packed[heads + mh], "sp", mh * group) for mh in range(heads)]
    hid_s = shared_gate.shape[1]
    width = 2 * gate_proj.shape[2]
    wide = (array(feats, width), array(feats, 2 * hid_s))
    laid_other, shared_other, shared_own = call(
        lay_kernel,
        wide + wide[1:],
        [smem()] + [hbm()] * 2 + [vmem()] * 4,
        [pltpu.SemaphoreType.DMA((2,))],
    )(at, in_hbm(shared_gate), in_hbm(shared_up), *others[1:5])
    *attended, out_w, laid_own = call(
        functools.partial(attention_kernel, heads=heads, group=group),
        (array(tok, hd),) * heads + (array(*out_proj.shape),) + wide[:1],
        [smem()] + [hbm()] * 3 + [vmem()] * (blocks + heads),
        [
            pltpu.VMEM((blocks, kv_rows, hd), BF),
            pltpu.VMEM((heads * tok, hd), BF),
            pltpu.VMEM((heads * tok, hd), F32),
            pltpu.VMEM((heads * tok, tok), F32),
            pltpu.SemaphoreType.DMA((3,)),
        ],
    )(
        at,
        *[in_hbm(x) for x in (out_proj, gate_proj, up_proj)],
        *kv,
        *q,
    )
    piece = call(stack_kernel, array(heads, tok, hd), [vmem()] * heads)(
        *[swap(attended[mh], "sp", mh * group) for mh in range(heads)]
    )
    bits = [1 << i for i in range(tp.bit_length() - 1)]
    pieces, masks = [piece], [0]
    for bit in reversed(bits):
        pieces = pieces + [swap(x, "tp", bit) for x in pieces]
        masks = masks + [m ^ bit for m in masks]

    local = gate_proj.shape[0]
    experts = local * blocks
    choices = expert_ids.shape[1]
    cap = 2 * choices * tok // experts
    mixed = call(
        functools.partial(project_kernel, masks=tuple(masks), heads=heads),
        array(tok, feats),
        [smem()] + [vmem()] * (len(pieces) + 2),
        [pltpu.VMEM((tok, out_proj.shape[0]), BF)],
    )(at, *pieces, out_w, stream)
    mixed_other = swap(mixed, "tp", 1)
    sends = call(
        functools.partial(dispatch_kernel, local=local),
        (array(2, cap, feats),) * blocks,
        [smem()] + [vmem()] * 3,
    )(at, expert_ids.T, mixed, mixed_other)

    half = blocks // 2
    quarter = half + half // 2
    groups = [range(half), range(half, quarter), range(quarter, blocks)]
    arrived = {m: swap(sends[m], "sp", m) for m in range(blocks)}

    shared_sum = call(
        shared_kernel, array(tok // 2, 2 * hid_s + LANES), [smem()] + [vmem()] * 6
    )(at, mixed, mixed_other, gain, others[0], shared_own, shared_other)

    def add(a, b, width):
        return call(functools.partial(add_kernel, width=width), array(*a.shape), [vmem()] * 2)(a, b)

    def hidden(a, b, width):
        return call(
            functools.partial(hidden_kernel, width=width, features=features),
            array(a.shape[0], width // 2),
            [vmem()] * 2,
        )(a, b)

    for bit in bits[1:-1]:
        other = swap(shared_sum, "tp", bit)
        shared_sum = add(shared_sum, other, 2 * hid_s)
    other = swap(shared_sum, "tp", bits[-1])
    shared_hidden = hidden(shared_sum, other, 2 * hid_s)
    other_hidden = swap(shared_hidden, "tp", 1)

    back = {}
    for ms in groups:
        total = call(
            routed_kernel, array(len(ms) * cap, width + LANES), [vmem()] * (len(ms) + 4)
        )(gain, others[0], laid_own, laid_other, *[arrived[m] for m in ms])
        for bit in bits[1:-1]:
            total = add(total, swap(total, "tp", bit), width)
        came = swap(total, "tp", bits[-1])
        outs = call(
            functools.partial(down_kernel, width=width, features=features),
            (array(2, cap, feats),) * len(ms),
            [smem()] + [vmem()] * 4,
        )(at, total, came, down_proj, others[5])
        for m, out in zip(ms, outs):
            back[m] = swap(out, "sp", m)
    total, *picks = call(
        functools.partial(base_kernel, local=local, cap=cap),
        (jax.ShapeDtypeStruct((2, tok, feats), F32),)
        + tuple(array(tok, 2 * len(ms) * cap) for ms in groups),
        [smem()] + [vmem()] * 6,
    )(at, expert_ids.T, route_weights.T, mixed, shared_hidden, other_hidden, shared_down)
    for i in (1, 0, 2):
        ms, last = groups[i], i == 2
        one = jax.ShapeDtypeStruct((tok, feats), F32)
        total = call(
            functools.partial(combine_kernel, outs=2 if last else 1),
            (one, array(tok, feats)) if last else jax.ShapeDtypeStruct((2, tok, feats), F32),
            [vmem()] * (2 + len(ms)),
        )(total, picks[i], *[back[m] for m in ms])
    return call(final_kernel, array(tok, feats), [vmem()] * 2)(total[0], swap(total[1], "tp", 1))


def solution(mesh):
    in_specs = (
        P("sp", "tp"),
        P("sp", "tp"),
        P("sp", "tp"),
        P("sp", "tp"),
        P("sp", "tp"),
        P(None, "tp"),
        P("tp"),
        P("sp", None),
        P("sp", None),
        P("sp", "tp", None),
        P("sp", "tp", None),
        P("sp", None, "tp"),
        P("tp", None),
        P("tp", None),
        P(None, "tp"),
    )
    out_specs = P("sp", "tp")
    return jax.shard_map(layer, mesh=mesh, in_specs=in_specs, out_specs=out_specs, check_vma=False)
```
